32 devices in a mesh: fs: 4 (over z), tp: 4 (over y, x), rep: 2 (over core).
Axes of the slice: x: 2, y: 2, z: 4, core: 2. Of those that a mesh axis runs over, the one named last changes fastest.
Arguments:
- gate_grads: float32 [2, 5632, 2048], P('rep', 'fs', 'tp'), may hold values from -16 to 16, as said below
- gate_velocity: float32 [5632, 2048], P(('fs', 'rep'), 'tp'), may hold values from -31 to 31, as said below
- gate_weight: float32 [5632, 2048], P(('fs', 'rep'), 'tp'), may hold values from -4 to 4
- up_grads: float32 [2, 5632, 2048], P('rep', 'fs', 'tp'), may hold values from -16 to 16, as said below
- up_velocity: float32 [5632, 2048], P(('fs', 'rep'), 'tp'), may hold values from -31 to 31, as said below
- up_weight: float32 [5632, 2048], P(('fs', 'rep'), 'tp'), may hold values from -4 to 4
- branch_grads: float32 [2, 2048, 1024], P('rep', 'fs', 'tp'), may hold values from -16 to 16, as said below
- branch_velocity: float32 [2048, 1024], P(('fs', 'rep'), 'tp'), may hold values from -31 to 31, as said below
- branch_weight: float32 [2048, 1024], P(('fs', 'rep'), 'tp'), may hold values from -4 to 4
Outputs:
- gate_momentum: float32 [5632, 2048], P(('fs', 'rep'), 'tp')
- gate_updated: float32 [5632, 2048], P(('fs', 'rep'), 'tp')
- up_momentum: float32 [5632, 2048], P(('fs', 'rep'), 'tp')
- up_updated: float32 [5632, 2048], P(('fs', 'rep'), 'tp')
- branch_momentum: float32 [2048, 1024], P(('fs', 'rep'), 'tp')
- branch_updated: float32 [2048, 1024], P(('fs', 'rep'), 'tp')
The draws below stay inside these ranges and needn't reach their ends.
Inputs may be any that keep to these rules, and one draw needn't show every extreme that they name: `gate_grads`: entries vary in scale over rows and over columns. `up_grads`: entries vary in scale over rows and over columns. `branch_grads`: entries vary in scale over rows and over columns. `gate_velocity`: entries vary in scale over rows and over columns. `up_velocity`: entries vary in scale over rows and over columns. `branch_velocity`: entries vary in scale over rows and over columns.
All inputs are finite; a program needn't handle non-finite values.
Results may differ from the reference program's by a relative error of at most 0.039.
Values may be sent and summed in bfloat16 or wider, within the bound.
No kernel may reach another device: no remote copies, remote signals or barrier semaphores. Data moves between devices by JAX's collectives and lax.ppermute only.
A program may use at most 64 MiB of HBM per device.

```python
import math
import jax
import jax.numpy as jnp
from jax import lax

D = 2048
FF = 5632
BRANCH = 1024
ITERS = 3
REP = 2
N_FS = 4
N_REP = 2


def block_scaled(key, height, width):
    noise_key, row_key, col_key = jax.random.split(key, 3)
    noise = jnp.clip(jax.random.normal(noise_key, (height, width), jnp.float32), -4.0, 4.0)
    rise = math.log(4.0)
    row_factor = jnp.exp(jax.random.uniform(row_key, (8,), jnp.float32, -0.3, 0.3))
    col_factor = jnp.exp(jax.random.uniform(col_key, (4,), jnp.float32, -0.3, 0.3))
    row_ramp = jnp.exp(rise * (jnp.arange(height, dtype=jnp.float32) / (height - 1) - 1.0))
    col_ramp = jnp.exp(rise * (jnp.arange(width, dtype=jnp.float32) / (width - 1) - 1.0))
    row_scale = jnp.repeat(row_factor, height // 8) * row_ramp
    col_scale = jnp.repeat(col_factor, width // 4) * col_ramp
    return noise * row_scale[:, None] * col_scale[None, :]


def replicas(key, height, width):
    return jnp.stack([block_scaled(jax.random.fold_in(key, 11 + index), height, width) for index in range(REP)])


def draw_gate_grads(key, part):
    return replicas(key, FF, D)


def draw_up_grads(key, part):
    return replicas(jax.random.fold_in(key, 3), FF, D)


def draw_branch_grads(key, part):
    return replicas(jax.random.fold_in(key, 5), D, BRANCH)


def draw_gate_velocity(key, part):
    return 2.0 * block_scaled(jax.random.fold_in(key, 21), FF, D)


def draw_up_velocity(key, part):
    return 2.0 * block_scaled(jax.random.fold_in(key, 23), FF, D)


def draw_branch_velocity(key, part):
    return 2.0 * block_scaled(jax.random.fold_in(key, 25), D, BRANCH)


def steps_of(key, extent, cuts, smallest, high):
    def one(dim, parts):
        steps = jax.random.uniform(jax.random.fold_in(jax.random.fold_in(key, 6), dim), (parts,), jnp.float32, smallest / len(cuts), high / len(cuts))
        return jnp.repeat(jnp.exp(steps), extent[dim] // parts).reshape((-1,) + (1,) * (len(extent) - dim - 1))

    gain = one(*cuts[0])
    for cut in cuts[1:]:
        gain = gain * one(*cut)
    return gain


def normal_values(own_key, shape, scale, most, shards=(), kind=jnp.bfloat16):
    array = jax.random.normal(own_key, shape, jnp.float32) * scale
    if len(shards) > 0:
        array = steps_of(own_key, shape, shards, -0.22, 0.18) * array
    return jnp.clip(array, min=-most, max=most).astype(kind)


def setup_inputs(seed: int = 0) -> dict:
    keys = jax.random.split(jax.random.key(seed), 10)
    return {
        "gate_grads": draw_gate_grads(jax.random.fold_in(keys[9], 71), 0),
        "gate_velocity": draw_gate_velocity(jax.random.fold_in(keys[9], 71), 0),
        "gate_weight": normal_values(keys[2], (FF, D), 1.0, 4.0, ((0, 8), (1, 4)), jnp.float32),
        "up_grads": draw_up_grads(jax.random.fold_in(keys[9], 71), 0),
        "up_velocity": draw_up_velocity(jax.random.fold_in(keys[9], 71), 0),
        "up_weight": normal_values(keys[5], (FF, D), 1.0, 4.0, ((0, 8), (1, 4)), jnp.float32),
        "branch_grads": draw_branch_grads(jax.random.fold_in(keys[9], 71), 0),
        "branch_velocity": draw_branch_velocity(jax.random.fold_in(keys[9], 71), 0),
        "branch_weight": normal_values(keys[8], (D, BRANCH), 1.0, 4.0, ((0, 8), (1, 4)), jnp.float32),
    }


MOMENT = 0.95
COEF_ONE = 3.4445
COEF_THREE = -4.775
COEF_FIVE = 2.0315
SAFETY = 2.0
RATE = 0.5
SHRINK = 0.95

def block_gram(matrix):
    count = N_FS * N_REP
    height = matrix.shape[0] // count
    width = matrix.shape[1]
    stacked = matrix.reshape(count, height, width)

    def add_block(total, block):
        part = jnp.dot(block.T, block, preferred_element_type=jnp.float32)
        narrow = lax.optimization_barrier(part.astype(jnp.bfloat16))
        return (total + narrow.astype(jnp.float32), None)
    total, unused = lax.scan(add_block, jnp.zeros((width, width), jnp.float32), stacked)
    return total

def orthogonal(momentum):
    start = momentum.astype(jnp.bfloat16)
    first = jnp.sum(jnp.square(start.astype(jnp.float32)))
    raw = block_gram(start)
    second = jnp.sum(raw * raw)
    ratio = SAFETY * (second + 1.0) / (first + 1.0)
    scale = lax.rsqrt(ratio)
    gram = (raw / ratio).astype(jnp.bfloat16)
    ymat = (jnp.dot(start, gram, preferred_element_type=jnp.float32) * scale).astype(jnp.bfloat16)
    zmat = jnp.dot(ymat, gram, preferred_element_type=jnp.float32).astype(jnp.bfloat16)
    current = (COEF_ONE * scale * start.astype(jnp.float32) + COEF_THREE * ymat.astype(jnp.float32) + COEF_FIVE * zmat.astype(jnp.float32)).astype(jnp.bfloat16)
    for index in range(ITERS - 1):
        gram = block_gram(current).astype(jnp.bfloat16)
        ymat = jnp.dot(current, gram, preferred_element_type=jnp.float32).astype(jnp.bfloat16)
        zmat = jnp.dot(ymat, gram, preferred_element_type=jnp.float32).astype(jnp.bfloat16)
        current = (COEF_ONE * current.astype(jnp.float32) + COEF_THREE * ymat.astype(jnp.float32) + COEF_FIVE * zmat.astype(jnp.float32)).astype(jnp.bfloat16)
    return current

def one_matrix(grads, velocity, weight):
    momentum = MOMENT * velocity + lax.optimization_barrier(jnp.sum(grads, axis=0))
    final = orthogonal(momentum)
    updated = SHRINK * weight - RATE * math.sqrt(weight.shape[0]) * final.astype(jnp.float32)
    return (momentum, updated)

def reference(gate_grads, gate_velocity, gate_weight, up_grads, up_velocity, up_weight, branch_grads, branch_velocity, branch_weight):
    gate_momentum, gate_updated = one_matrix(gate_grads, gate_velocity, gate_weight)
    up_momentum, up_updated = one_matrix(up_grads, up_velocity, up_weight)
    branch_momentum, branch_updated = one_matrix(branch_grads, branch_velocity, branch_weight)
    return (gate_momentum, gate_updated, up_momentum, up_updated, branch_momentum, branch_updated)
```

```python
import functools
import math

import jax
import jax.numpy as jnp
from jax import lax
from jax.experimental import pallas as pl
from jax.experimental.pallas import tpu as pltpu
from jax.sharding import PartitionSpec as P

MOMENT = 0.95
COEF_ONE = 3.4445
COEF_THREE = -4.775
COEF_FIVE = 2.0315
SAFETY = 2.0
RATE = 0.5
SHRINK = 0.95


BF16 = jnp.bfloat16
F32 = jnp.float32


def swap(size, bit):
    return [(i, i ^ bit) for i in range(size)]


def shift(size, step):
    return [(i, (i + step) % size) for i in range(size)]


def dot(left, right):
    return jnp.dot(left, right, preferred_element_type=F32)


def chain_kernel(f_count, place_ref, *refs):
    count = 4 * f_count
    pieces = refs[:count]
    out_ref = refs[count]
    panel, buf, col, sem = refs[count + 1 :]
    n = buf.shape[1]
    nb = n // 4
    half = nb // 2
    me = place_ref[0]
    row = place_ref[1]
    copies = []
    for b in range(4):
        for s in range(f_count):
            piece = pieces[b * f_count + s]
            height = piece.shape[0]
            slot = lax.rem(row + (f_count - s), f_count)
            start = pl.multiple_of(slot * height, height)
            copies.append(
                pltpu.make_async_copy(
                    piece, panel.at[b, pl.ds(start, height), :], sem.at[b * f_count + s]
                )
            )
    for copy in copies:
        copy.start()
    for copy in copies:
        copy.wait()

    bit_x = lax.rem(me, 2)
    bit_y = lax.div(me, 2)
    eye = lax.broadcasted_iota(jnp.int32, (nb, nb), 0) == lax.broadcasted_iota(
        jnp.int32, (nb, nb), 1
    )
    trace = jnp.zeros((1, 1), F32)
    for b in range(4):
        block = panel[b, 0:nb, :]
        buf[0, b * nb : (b + 1) * nb, b * nb : (b + 1) * nb] = block
        picked = jnp.where(eye, block.astype(F32), 0.0)
        trace = trace + jnp.sum(picked, keepdims=True)
        bx, by = b & 1, b >> 1
        own_x = bit_x ^ bx
        own_y = bit_y ^ by
        pairs = (
            (own_x, b ^ 1, b),
            (own_y, b ^ 2, b),
            (own_y, b ^ 2, b ^ 1),
        )
        for index, (flag, high, low) in enumerate(pairs):
            part = panel[b, nb + index * half : nb + (index + 1) * half, :]
            tall = jnp.where(flag == 0, high, low)
            wide = jnp.where(flag == 0, low, high)
            rows = pl.multiple_of(tall * nb + flag * half, half)
            cols = pl.multiple_of(wide * nb, nb)
            buf[0, pl.ds(rows, half), pl.ds(cols, nb)] = part
            buf[0, pl.ds(cols, nb), pl.ds(rows, half)] = part.T

    def add_square(i, total):
        part = buf[0, pl.ds(pl.multiple_of(i * nb, nb), nb), :].astype(F32)
        return total + jnp.sum(part * part, keepdims=True)

    second = lax.fori_loop(0, 4, add_square, jnp.zeros((1, 1), F32))
    ratio = SAFETY * (second + 1.0) / (trace + 1.0)
    inverse = 1.0 / ratio
    scale = lax.rsqrt(ratio)

    one = jnp.ones((1, 1), F32)

    def product(step, carry):
        which = lax.div(step, 16)
        i = lax.rem(lax.div(step, 4), 4)
        j = lax.rem(step, 4)
        left = jnp.where(which == 2, 2, 0)
        right = jnp.where((which == 1) | (which == 2), 1, 0)
        into = jnp.where(which == 0, 1, jnp.where(which == 2, 0, 2))
        linear = jnp.where((which == 0) | (which == 3), COEF_THREE, COEF_ONE) * jnp.where(
            which < 2, inverse, one
        )
        quad = jnp.where((which == 0) | (which == 3), COEF_FIVE, 1.0) * jnp.where(
            which == 0, inverse * inverse, jnp.where(which == 1, inverse, one)
        )
        rows = pl.ds(pl.multiple_of(i * nb, nb), nb)
        cols = pl.ds(pl.multiple_of(j * nb, nb), nb)
        acc = dot(buf[left, rows, :], buf[right, :, cols])
        base = buf[left, rows, cols].astype(F32)
        buf[into, rows, cols] = (linear * base + quad * acc).astype(BF16)
        return carry

    lax.fori_loop(0, 64, product, 0)

    unit = jnp.where(eye, 1.0, 0.0)
    col[0] = buf[2, :, 0:nb]
    col[0, 0:nb, :] = (buf[2, 0:nb, 0:nb].astype(F32) + COEF_ONE * unit).astype(BF16)
    col[2] = jnp.zeros((n, nb), BF16)

    def column(step, carry):
        which = lax.div(step, 4)
        i = lax.rem(step, 4)
        matrix = jnp.where((which == 1) | (which == 4), 0, 2)
        source = jnp.where(
            which == 2, 2, jnp.where((which == 0) | (which == 3) | (which == 5), 0, 1)
        )
        into = jnp.where(which == 1, 2, jnp.where((which == 2) | (which == 4), 0, 1))
        alpha = jnp.where((which == 1) | (which == 4), 0.0, COEF_ONE)
        beta = jnp.where(which == 4, COEF_FIVE, 1.0)
        gamma = jnp.where(which == 4, COEF_THREE, 0.0)
        delta = jnp.where((which == 4) & (i == 0), COEF_ONE, 0.0)
        rows = pl.ds(pl.multiple_of(i * nb, nb), nb)
        acc = dot(buf[matrix, rows, :], col[source])
        value = alpha * col[source, rows, :].astype(F32) + beta * acc
        value = value + gamma * col[2, rows, :].astype(F32) + delta * unit
        col[into, rows, :] = value.astype(BF16)
        return carry

    lax.fori_loop(0, 24, column, 0)

    def last(i, carry):
        rows = pl.ds(pl.multiple_of(i * nb, nb), nb)
        acc = dot(buf[1, rows, :], col[1])
        value = scale * (COEF_ONE * col[1, rows, :].astype(F32) + acc)
        out_ref[rows, :] = value.astype(BF16)
        return carry

    lax.fori_loop(0, 4, last, 0)


def chain(pieces, place, f_count, n):
    nb = n // 4
    flat = [piece for group in pieces for piece in group]
    flops = int((4.0 + 1.75) * 2 * n**3)
    return pl.pallas_call(
        functools.partial(chain_kernel, f_count),
        out_shape=jax.ShapeDtypeStruct((n, nb), BF16),
        in_specs=[pl.BlockSpec(memory_space=pltpu.SMEM)]
        + [pl.BlockSpec(memory_space=pl.ANY)] * len(flat),
        out_specs=pl.BlockSpec(memory_space=pltpu.VMEM),
        scratch_shapes=[
            pltpu.VMEM((4, 5 * half_of(nb), nb), BF16),
            pltpu.VMEM((3, n, n), BF16),
            pltpu.VMEM((3, n, nb), BF16),
            pltpu.SemaphoreType.DMA((4 * f_count,)),
        ],
        compiler_params=pltpu.CompilerParams(vmem_limit_bytes=56 * 1024 * 1024),
        cost_estimate=pl.CostEstimate(flops=flops, bytes_accessed=6 * n * nb, transcendentals=0),
    )(place, *flat)


def half_of(width):
    return width // 2


def apply_kernel(a_ref, b_ref, c_ref, d_ref, q_ref, out_ref):
    nb = a_ref.shape[1]
    total = dot(a_ref[...], q_ref[0:nb, :])
    for index, ref in enumerate((b_ref, c_ref, d_ref)):
        total = total + dot(ref[...], q_ref[(index + 1) * nb : (index + 2) * nb, :])
    out_ref[...] = total.astype(BF16)


def apply(blocks, q):
    rows, nb = blocks[0].shape
    return pl.pallas_call(
        apply_kernel,
        out_shape=jax.ShapeDtypeStruct((rows, nb), BF16),
        cost_estimate=pl.CostEstimate(
            flops=8 * rows * nb * nb, bytes_accessed=18 * rows * nb, transcendentals=0
        ),
    )(*blocks, q)


def transposed_dot(left, right):
    return lax.dot_general(left, right, (((0,), (0,)), ((), ())), preferred_element_type=F32)


def panel_of(own, along_x, along_y, bit_x, bit_y):
    half = own.shape[1] // 2
    parts = [transposed_dot(own, own)]
    parts.append(
        transposed_dot(
            jnp.where(bit_x == 0, along_x[:, :half], own[:, half:]),
            jnp.where(bit_x == 0, own, along_x),
        )
    )
    parts.append(
        transposed_dot(
            jnp.where(bit_y == 0, along_y[:, :half], own[:, half:]),
            jnp.where(bit_y == 0, own, along_y),
        )
    )
    parts.append(
        transposed_dot(
            jnp.where(bit_y == 0, along_y[:, :half], along_x[:, half:]),
            jnp.where(bit_y == 0, along_x, along_y),
        )
    )
    return jnp.concatenate([part.astype(BF16) for part in parts], axis=0)


def reduce_rows(panel, axis, size, place):
    height = panel.shape[0] // size
    total = lax.dynamic_slice_in_dim(panel, place * height, height, 0).astype(F32)
    for step in range(1, size):
        piece = lax.dynamic_slice_in_dim(
            panel, lax.rem(place + step, size) * height, height, 0
        )
        total = total + lax.ppermute(piece, axis, shift(size, step)).astype(F32)
    return total.astype(BF16)


def spread(piece, axis, size):
    return [piece] + [lax.ppermute(piece, axis, shift(size, step)) for step in range(1, size)]


def local(f_size, *arrays):
    gate, up, branch = arrays[0:3], arrays[3:6], arrays[6:9]
    rep = lax.axis_index("rep")
    tp = lax.axis_index("tp")
    fs = lax.axis_index("fs")
    bit_x = lax.rem(tp, 2)
    bit_y = lax.div(tp, 2)
    place = jnp.stack([tp, fs]).astype(jnp.int32)

    moments = []
    for grads, velocity, weight in (branch, gate, up):
        height = velocity.shape[0]
        theirs = lax.dynamic_slice_in_dim(grads[0], (1 - rep) * height, height, 0)
        mine = lax.dynamic_slice_in_dim(grads[0], rep * height, height, 0)
        received = lax.ppermute(theirs.astype(BF16), "rep", swap(2, 1))
        moments.append(MOMENT * velocity + (mine + received.astype(F32)))
    starts = [moment.astype(BF16) for moment in moments]

    keep = jnp.where(rep == 0, starts[1], starts[2])
    give = jnp.where(rep == 0, starts[2], starts[1])
    both = jnp.concatenate([keep, lax.ppermute(give, "rep", swap(2, 1))], axis=0)
    small = starts[0]

    small_x = lax.ppermute(small, "tp", swap(4, 1))
    small_y = lax.ppermute(small, "tp", swap(4, 2))
    both_x = lax.ppermute(both, "tp", swap(4, 1))
    both_y = lax.ppermute(both, "tp", swap(4, 2))

    small_panel = panel_of(small, small_x, small_y, bit_x, bit_y)
    height = small_panel.shape[0] // 2
    mine = lax.dynamic_slice_in_dim(small_panel, rep * height, height, 0)
    theirs = lax.dynamic_slice_in_dim(small_panel, (1 - rep) * height, height, 0)
    mine = mine.astype(F32) + lax.ppermute(theirs, "rep", swap(2, 1)).astype(F32)
    piece = reduce_rows(mine.astype(BF16), "fs", f_size, fs)
    parts = spread(piece, "fs", f_size)
    ordered = jnp.concatenate((parts[::-1]) * 2, axis=0)
    whole = lax.dynamic_slice_in_dim(
        ordered, lax.rem(2 * f_size - 1 - fs, f_size) * piece.shape[0], height, 0
    )
    spreads = jnp.stack([whole] + [lax.ppermute(whole, "tp", swap(4, b)) for b in (1, 2, 3)])
    others = lax.ppermute(spreads, "rep", swap(2, 1))
    small_full = jnp.where(
        rep == 0,
        jnp.concatenate([spreads, others], axis=1),
        jnp.concatenate([others, spreads], axis=1),
    )

    panel = panel_of(both, both_x, both_y, bit_x, bit_y)
    piece = reduce_rows(panel, "fs", f_size, fs)
    parts = spread(piece, "fs", f_size)
    groups = [parts]
    for b in (1, 2, 3):
        groups.append([lax.ppermute(part, "tp", swap(4, b)) for part in parts])

    small_q = chain([[small_full[b]] for b in range(4)], place, 1, 4 * small.shape[1])
    both_q = chain(groups, place, f_size, 4 * both.shape[1])

    small_d = lax.ppermute(small, "tp", swap(4, 3))
    both_d = lax.ppermute(both, "tp", swap(4, 3))
    rows = keep.shape[0]
    blocks = (both, both_x, both_y, both_d)
    sent = apply([block[rows:] for block in blocks], both_q)
    arrived = lax.ppermute(sent, "rep", swap(2, 1))
    kept = apply([block[:rows] for block in blocks], both_q)
    small_out = apply([small, small_x, small_y, small_d], small_q)

    finals = (
        jnp.where(rep == 0, kept, arrived),
        jnp.where(rep == 0, arrived, kept),
        small_out,
    )
    results = []
    order = (moments[1], moments[2], moments[0])
    for moment, final, weight, height in zip(
        order, finals, (gate[2], up[2], branch[2]), HEIGHTS(f_size, arrays)
    ):
        results.append(moment)
        results.append(SHRINK * weight - RATE * math.sqrt(height) * final.astype(F32))
    return tuple(results)


def HEIGHTS(f_size, arrays):
    return [arrays[3 * k].shape[1] * f_size for k in range(3)]


def solution(mesh):
    grads = P("rep", "fs", "tp")
    state = P(("fs", "rep"), "tp")
    return jax.shard_map(
        functools.partial(local, mesh.shape["fs"]),
        mesh=mesh,
        in_specs=(grads, state, state) * 3,
        out_specs=(state,) * 6,
        check_vma=False,
    )
```

```python
import functools
import math

import jax
import jax.numpy as jnp
from jax import lax
from jax.experimental import pallas as pl
from jax.experimental.pallas import tpu as pltpu
from jax.sharding import PartitionSpec as P


MOMENT = 0.95
COEF_ONE = 3.4445
COEF_THREE = -4.775
COEF_FIVE = 2.0315
SAFETY = 2.0
RATE = 0.5
SHRINK = 0.95


BF16 = jnp.bfloat16
F32 = jnp.float32


def swap(size, bit):
    return [(i, i ^ bit) for i in range(size)]


def shift(size, step):
    return [(i, (i + step) % size) for i in range(size)]


def dot(left, right):
    return jnp.dot(left, right, preferred_element_type=F32)


def unfold(size, place_ref, arrays, panel):
    rep = place_ref[2]
    fold = arrays[0].shape[1]
    nb = panel.shape[2]
    turn = (place_ref[1] + 1) * (fold // size)
    for array, side in ((arrays[0], rep), (arrays[1], 1 - rep)):
        for b in range(4):
            value = pltpu.roll(array[b].astype(F32), turn, 0).astype(BF16)
            for half in range(2):
                start = pl.multiple_of((2 * side + half) * fold, 16)
                panel[b, pl.ds(start, fold), :] = value[:, half * nb : (half + 1) * nb]


def chain_kernel(plan, size, tile, place_ref, *refs):
    count = len(refs) - 5
    arrays = refs[:count]
    out_ref, panel, buf, col, sem = refs[count:]
    n = buf.shape[1]
    nb = n // 4
    half = nb // 2
    edge = n // tile
    me = place_ref[0]
    row = place_ref[1]
    if plan is None:
        unfold(size, place_ref, arrays, panel)
    copies = []
    for index, (b, array, source, height, base, period, step) in enumerate(plan or ()):
        slot = lax.rem(row + (size - step), size)
        start = pl.multiple_of(base + slot * period, 16)
        copies.append(
            pltpu.make_async_copy(
                arrays[array].at[pl.ds(source, height), :],
                panel.at[b, pl.ds(start, height), :],
                sem.at[index],
            )
        )
    for copy in copies:
        copy.start()
    for copy in copies:
        copy.wait()

    bit_x = lax.rem(me, 2)
    bit_y = lax.div(me, 2)
    eye = lax.broadcasted_iota(jnp.int32, (tile, nb), 0) == lax.broadcasted_iota(
        jnp.int32, (tile, nb), 1
    )
    trace = jnp.zeros((1, 1), F32)
    for b in range(4):
        block = panel[b, 0:nb, :]
        buf[0, b * nb : (b + 1) * nb, b * nb : (b + 1) * nb] = block
        picked = jnp.where(eye[0:nb], block.astype(F32), 0.0)
        trace = trace + jnp.sum(picked, keepdims=True)
        own_x = bit_x ^ (b & 1)
        own_y = bit_y ^ (b >> 1)
        pairs = ((own_x, b ^ 1, b), (own_y, b ^ 2, b), (own_y, b ^ 2, b ^ 1))
        for index, (flag, high, low) in enumerate(pairs):
            part = panel[b, nb + index * half : nb + (index + 1) * half, :]
            tall = jnp.where(flag == 0, high, low)
            wide = jnp.where(flag == 0, low, high)
            rows = pl.multiple_of(tall * nb + flag * half, half)
            cols = pl.multiple_of(wide * nb, nb)
            buf[0, pl.ds(rows, half), pl.ds(cols, nb)] = part
            buf[0, pl.ds(cols, nb), pl.ds(rows, half)] = part.T

    def add_square(i, total):
        part = buf[0, pl.ds(pl.multiple_of(i * tile, tile), tile), :].astype(F32)
        return total + jnp.sum(part * part, keepdims=True)

    second = lax.fori_loop(0, edge, add_square, jnp.zeros((1, 1), F32))
    ratio = SAFETY * (second + 1.0) / (trace + 1.0)
    inverse = 1.0 / ratio
    scale = lax.rsqrt(ratio)
    one = jnp.ones((1, 1), F32)

    cells = [(i, j) for j in range(edge) for i in range(j, edge)]

    def product(step, carry):
        which = lax.div(step, len(cells))
        cell = lax.rem(step, len(cells))
        i = jnp.int32(0)
        j = jnp.int32(0)
        for index, (a, b) in enumerate(cells):
            i = jnp.where(cell == index, a, i)
            j = jnp.where(cell == index, b, j)
        square = (which == 0) | (which == 3)
        left = jnp.where(which == 2, 2, 0)
        right = jnp.where(square, 0, jnp.where(which == 4, 2, 1))
        into = jnp.where(
            which == 0, 1, jnp.where(which == 2, 0, jnp.where(which == 4, 3, 2))
        )
        linear = jnp.where(square, COEF_THREE, COEF_ONE) * jnp.where(which < 2, inverse, one)
        quad = jnp.where(square, COEF_FIVE, 1.0) * jnp.where(
            which == 0, inverse * inverse, jnp.where(which == 1, inverse, one)
        )
        rows = pl.ds(pl.multiple_of(i * tile, tile), tile)
        cols = pl.ds(pl.multiple_of(j * tile, tile), tile)
        acc = dot(buf[left, rows, :], buf[right, :, cols])
        value = (linear * buf[left, rows, cols].astype(F32) + quad * acc).astype(BF16)
        buf[into, rows, cols] = value

        @pl.when(i != j)
        def _():
            buf[into, cols, rows] = value.T

        return carry

    lax.fori_loop(0, 5 * len(cells), product, 0)

    unit = jnp.where(eye, 1.0, 0.0)
    col[0] = buf[2, :, 0:nb]
    col[0, 0:nb, :] = (buf[2, 0:nb, 0:nb].astype(F32) + COEF_ONE * unit[0:nb]).astype(BF16)
    col[2] = jnp.zeros((n, nb), BF16)

    def column(step, carry):
        which = lax.div(step, edge)
        i = lax.rem(step, edge)
        matrix = jnp.where((which == 0) | (which == 2), 3, 2)
        source = jnp.where(which == 1, 2, jnp.where(which == 2, 1, 0))
        into = jnp.where(which == 0, 2, jnp.where(which == 2, 0, 1))
        alpha = jnp.where((which == 0) | (which == 2), 0.0, COEF_ONE)
        beta = jnp.where(which == 2, COEF_FIVE, 1.0)
        gamma = jnp.where(which == 2, COEF_THREE, 0.0)
        delta = jnp.where((which == 2) & (i == 0), COEF_ONE, 0.0)
        rows = pl.ds(pl.multiple_of(i * tile, tile), tile)
        acc = dot(buf[matrix, rows, :], col[source])
        value = alpha * col[source, rows, :].astype(F32) + beta * acc
        value = value + gamma * col[2, rows, :].astype(F32) + delta * unit
        col[into, rows, :] = value.astype(BF16)
        return carry

    lax.fori_loop(0, 4 * edge, column, 0)

    def last(i, carry):
        rows = pl.ds(pl.multiple_of(i * tile, tile), tile)
        acc = dot(buf[1, rows, :], col[1])
        value = scale * (COEF_ONE * col[1, rows, :].astype(F32) + acc)
        out_ref[rows, :] = value.astype(BF16)
        return carry

    lax.fori_loop(0, edge, last, 0)


def chain(plan, arrays, place, size, n):
    nb = n // 4
    tile = min(n, 512)
    flops = int(5.0 * 2 * n**3)
    return pl.pallas_call(
        functools.partial(chain_kernel, plan, size, tile),
        out_shape=jax.ShapeDtypeStruct((n, nb), BF16),
        in_specs=[pl.BlockSpec(memory_space=pltpu.SMEM)]
        + [pl.BlockSpec(memory_space=pl.ANY if plan else pltpu.VMEM)] * len(arrays),
        out_specs=pl.BlockSpec(memory_space=pltpu.VMEM),
        scratch_shapes=[
            pltpu.VMEM((4, 5 * nb // 2, nb), BF16),
            pltpu.VMEM((4, n, n), BF16),
            pltpu.VMEM((3, n, nb), BF16),
            pltpu.SemaphoreType.DMA((len(plan or (0,)),)),
        ],
        compiler_params=pltpu.CompilerParams(
            vmem_limit_bytes=min(56, 8 + 24 * n * n // 2**20 // 2) * 2**20
        ),
        cost_estimate=pl.CostEstimate(flops=flops, bytes_accessed=6 * n * nb, transcendentals=0),
    )(place, *arrays)


def apply_kernel(a_ref, b_ref, c_ref, d_ref, q_ref, out_ref):
    nb = a_ref.shape[1]
    total = dot(a_ref[...], q_ref[0:nb, :])
    for index, ref in enumerate((b_ref, c_ref, d_ref)):
        total = total + dot(ref[...], q_ref[(index + 1) * nb : (index + 2) * nb, :])
    out_ref[...] = total.astype(BF16)


def apply(blocks, q):
    rows, nb = blocks[0].shape
    step = rows // 2 if rows % 32 == 0 else rows
    block = pl.BlockSpec((step, nb), lambda i: (i, 0))
    return pl.pallas_call(
        apply_kernel,
        grid=(rows // step,),
        in_specs=[block] * 4 + [pl.BlockSpec((4 * nb, nb), lambda i: (0, 0))],
        out_specs=block,
        out_shape=jax.ShapeDtypeStruct((rows, nb), BF16),
        compiler_params=pltpu.CompilerParams(vmem_limit_bytes=16 * 2**20),
        cost_estimate=pl.CostEstimate(
            flops=8 * rows * nb * nb, bytes_accessed=18 * rows * nb, transcendentals=0
        ),
    )(*blocks, q)


def own_kernel(*refs):
    out_ref = refs[-1]
    total = None
    for ref in refs[:-1]:
        value = ref[...]
        part = dot(value.T, value)
        total = part if total is None else total + part
    out_ref[...] = total.astype(BF16)


def own_gram(blocks):
    nb = blocks[0].shape[1]
    flops = sum(2 * block.shape[0] * nb * nb for block in blocks)
    return pl.pallas_call(
        own_kernel,
        out_shape=jax.ShapeDtypeStruct((nb, nb), BF16),
        compiler_params=pltpu.CompilerParams(vmem_limit_bytes=16 * 2**20),
        cost_estimate=pl.CostEstimate(flops=flops, bytes_accessed=2**20, transcendentals=0),
    )(*blocks)


def cross_kernel(count, place_ref, *refs):
    own, along_x, along_y = refs[0:count], refs[count : 2 * count], refs[2 * count : 3 * count]
    out_ref = refs[-1]
    half = out_ref.shape[1] // 2
    bit_x = lax.rem(place_ref[0], 2)
    bit_y = lax.div(place_ref[0], 2)

    def part(index, left, column, right):
        total = None
        for l_ref, r_ref in zip(left, right):
            value = dot(l_ref[:, column * half : (column + 1) * half].T, r_ref[...])
            total = value if total is None else total + value
        out_ref[index * half : (index + 1) * half, :] = total.astype(BF16)

    @pl.when(bit_x == 0)
    def _():
        part(0, along_x, 0, own)

    @pl.when(bit_x == 1)
    def _():
        part(0, own, 1, along_x)

    @pl.when(bit_y == 0)
    def _():
        part(1, along_y, 0, own)
        part(2, along_y, 0, along_x)

    @pl.when(bit_y == 1)
    def _():
        part(1, own, 1, along_y)
        part(2, along_x, 1, along_y)


def cross_gram(own, along_x, along_y, place):
    nb = own[0].shape[1]
    arrays = (*own, *along_x, *along_y)
    flops = sum(3 * block.shape[0] * nb * nb for block in own)
    return pl.pallas_call(
        functools.partial(cross_kernel, len(own)),
        out_shape=jax.ShapeDtypeStruct((3 * nb // 2, nb), BF16),
        in_specs=[pl.BlockSpec(memory_space=pltpu.SMEM)]
        + [pl.BlockSpec(memory_space=pltpu.VMEM)] * len(arrays),
        out_specs=pl.BlockSpec(memory_space=pltpu.VMEM),
        compiler_params=pltpu.CompilerParams(vmem_limit_bytes=24 * 2**20),
        cost_estimate=pl.CostEstimate(flops=flops, bytes_accessed=2**20, transcendentals=0),
    )(place, *arrays)


def scatter(chunk, size, place):
    return [
        lax.ppermute(chunk(lax.rem(place + step, size)), "fs", shift(size, step))
        for step in range(1, size)
    ]


def add_up(own, moved):
    total = own.astype(F32)
    for value in moved:
        total = total + value.astype(F32)
    return total.astype(BF16)


def spread(piece, size):
    return [lax.ppermute(piece, "fs", shift(size, step)) for step in range(1, size)]


def around(value):
    return [value] + [lax.ppermute(value, "tp", swap(4, b)) for b in (1, 2, 3)]


def pack_kernel(part, *refs):
    values = refs[:-2]
    out_ref = refs[-1]
    count = len(values)
    tail = values[0].shape[0] - part
    for index, ref in enumerate(values):
        out_ref[index * part : (index + 1) * part, :] = ref[0:part, :]
        if tail:
            start = count * part + (count - 1 - index) * tail
            out_ref[start : start + tail, :] = ref[part:, :]


def pack(values, later, part):
    rows = sum(value.shape[0] for value in values)
    return pl.pallas_call(
        functools.partial(pack_kernel, part),
        out_shape=jax.ShapeDtypeStruct((rows, values[0].shape[1]), BF16),
        in_specs=[pl.BlockSpec(memory_space=pltpu.VMEM)] * len(values)
        + [pl.BlockSpec(memory_space=pl.ANY)],
        out_specs=pl.BlockSpec(memory_space=pltpu.VMEM),
        compiler_params=pltpu.CompilerParams(vmem_limit_bytes=16 * 2**20),
    )(*values, later)


def relay(value, split):
    along_x = lax.ppermute(value, "tp", swap(4, 1))
    along_y = lax.ppermute(value, "tp", swap(4, 2))
    upper, lower = along_y[:split], along_x[split:]
    upper = lax.ppermute(upper, "tp", swap(4, 1))
    lower = lax.ppermute(lower, "tp", swap(4, 2))
    return [value, along_x, along_y, upper, lower]


def half_sum(grads, rep):
    height = grads.shape[1] // 2
    theirs = lax.dynamic_slice_in_dim(grads[0], (1 - rep) * height, height, 0)
    mine = lax.dynamic_slice_in_dim(grads[0], rep * height, height, 0)
    return mine, theirs.astype(BF16)


def local(f_size, *arrays):
    return update(f_size, *arrays)


def update(f_size, *arrays):
    rep = lax.axis_index("rep")
    tp = lax.axis_index("tp")
    fs = lax.axis_index("fs")
    place = jnp.stack([tp, fs, rep]).astype(jnp.int32)
    velocities = arrays[1::3]
    weights = arrays[2::3]
    heights = [arrays[3 * k].shape[1] * f_size for k in range(3)]
    cross = swap(2, 1)

    halves = [half_sum(arrays[3 * k], rep) for k in range(3)]
    received = [lax.ppermute(halves[k][1], "rep", cross) for k in range(3)]
    moments = [
        MOMENT * velocities[k] + (halves[k][0] + received[k].astype(F32)) for k in range(3)
    ]
    starts = [moment.astype(BF16) for moment in moments]
    small = starts[2]

    keep = jnp.where(rep == 0, starts[0], starts[1])
    give = jnp.where(rep == 0, starts[1], starts[0])
    small_x = lax.ppermute(small, "tp", swap(4, 1))
    small_y = lax.ppermute(small, "tp", swap(4, 2))
    small_d = lax.ppermute(small, "tp", swap(4, 3))
    keep_x = lax.ppermute(keep, "tp", swap(4, 1))
    keep_y = lax.ppermute(keep, "tp", swap(4, 2))
    gift = lax.ppermute(give, "rep", cross)
    gift_x = lax.ppermute(gift, "tp", swap(4, 1))
    gift_y = lax.ppermute(gift, "tp", swap(4, 2))

    small_panel = jnp.concatenate(
        [own_gram([small]), cross_gram([small], [small_x], [small_y], place)], axis=0
    )
    height = small_panel.shape[0] // 2
    fold = height // 2
    mine = lax.dynamic_slice_in_dim(small_panel, rep * height, height, 0)
    theirs = lax.dynamic_slice_in_dim(small_panel, (1 - rep) * height, height, 0)
    mine = mine.astype(F32) + lax.ppermute(theirs, "rep", cross).astype(F32)
    mine = mine.astype(BF16)
    mine = jnp.concatenate([mine[:fold], mine[fold:]], axis=1)
    diagonal = own_gram([keep, gift])
    nb = diagonal.shape[0]
    part = nb // f_size
    tail = fold // f_size

    def chunk(index):
        return jnp.concatenate(
            [
                lax.dynamic_slice_in_dim(diagonal, index * part, part, 0),
                lax.dynamic_slice_in_dim(mine, index * tail, tail, 0),
            ],
            axis=0,
        )

    total = add_up(chunk(fs), scatter(chunk, f_size, fs))
    parts = [total] + spread(total, f_size)
    rest = cross_gram([keep, gift], [keep_x, gift_x], [keep_y, gift_y], place)
    height = rest.shape[0] // f_size

    def slab(index):
        return lax.dynamic_slice_in_dim(rest, index * height, height, 0)

    moved = scatter(slab, f_size, fs)
    first_parts = pack(parts, rest, part)
    piece = add_up(slab(fs), moved)
    split = first_parts.shape[0] // 32 * 16
    first_groups = relay(first_parts, split)
    rest_parts = spread(piece, f_size)
    own_groups = around(piece)
    rest_parts = pack(rest_parts, piece, height)
    rest_groups = around(rest_parts)
    spreads = jnp.stack([group[nb:] for group in first_groups[:3]] + [first_groups[4][nb - split :]])
    others = lax.ppermute(spreads, "rep", cross)
    n = 4 * small.shape[1]
    small_q = chain(None, [spreads, others], place, f_size, n)
    small_out = apply([small, small_x, small_y, small_d], small_q)

    own_groups, rest_groups, first_groups, small_out, keep, gift = lax.optimization_barrier(
        (own_groups, rest_groups, first_groups, small_out, keep, gift)
    )
    n = 4 * nb
    plan = []
    for b in range(4):
        for step in range(f_size):
            low, high = step * part, (step + 1) * part
            if b < 3 or high <= split:
                plan.append((b, b, low, part, 0, part, step))
            elif low >= split:
                plan.append((b, 4, low - split, part, 0, part, step))
            else:
                plan.append((b, 3, low, split - low, 0, part, step))
                plan.append((b, 4, 0, high - split, split - low, part, step))
        plan.append((b, 5 + b, 0, height, nb, height, 0))
        for step in range(1, f_size):
            plan.append((b, 9 + b, (step - 1) * height, height, nb, height, step))
    both_q = chain(plan, [*first_groups, *own_groups, *rest_groups], place, f_size, n)

    gift_d = lax.ppermute(gift, "tp", swap(4, 3))
    keep_d = lax.ppermute(keep, "tp", swap(4, 3))
    sent = apply([gift, gift_x, gift_y, gift_d], both_q)
    arrived = lax.ppermute(sent, "rep", cross)
    kept = apply([keep, keep_x, keep_y, keep_d], both_q)
    finals = (
        jnp.where(rep == 0, kept, arrived),
        jnp.where(rep == 0, arrived, kept),
        small_out,
    )
    results = []
    for moment, final, weight, rows in zip(moments, finals, weights, heights):
        results.append(moment)
        results.append(SHRINK * weight - RATE * math.sqrt(rows) * final.astype(F32))
    return tuple(results)


def solution(mesh):
    grads = P("rep", "fs", "tp")
    state = P(("fs", "rep"), "tp")
    f_size = mesh.shape["fs"]
    return jax.shard_map(
        functools.partial(local, f_size),
        mesh=mesh,
        in_specs=(grads, state, state) * 3,
        out_specs=(state,) * 6,
        check_vma=False,
    )
```

```python
import functools
import math

import jax
import jax.numpy as jnp
from jax import lax
from jax.experimental import pallas as pl
from jax.experimental.pallas import tpu as pltpu
from jax.sharding import PartitionSpec as P


MOMENT = 0.95
COEF_ONE = 3.4445
COEF_THREE = -4.775
COEF_FIVE = 2.0315
SAFETY = 2.0
RATE = 0.5
SHRINK = 0.95


BF16 = jnp.bfloat16
F32 = jnp.float32


def swap(size, bit):
    return [(i, i ^ bit) for i in range(size)]


def shift(size, step):
    return [(i, (i + step) % size) for i in range(size)]


def dot(left, right):
    return jnp.dot(left, right, preferred_element_type=F32)


def unfold(size, place_ref, arrays, panel):
    rep = place_ref[2]
    fold = arrays[0].shape[1]
    nb = panel.shape[2]
    turn = (place_ref[1] + 1) * (fold // size)
    for array, side in ((arrays[0], rep), (arrays[1], 1 - rep)):
        for b in range(4):
            value = pltpu.roll(array[b].astype(F32), turn, 0).astype(BF16)
            for half in range(2):
                start = pl.multiple_of((2 * side + half) * fold, 16)
                panel[b, pl.ds(start, fold), :] = value[:, half * nb : (half + 1) * nb]


def chain_kernel(plan, size, tile, place_ref, *refs):
    arrays = refs[:-12]
    out_ref, panel, raw, one, two, three, col_a, col_b, col_c, acc_a, acc_b, sem = refs[-12:]
    n = raw.shape[0]
    nb = n // 4
    half = nb // 2
    edge = n // tile
    me = place_ref[0]
    row = place_ref[1]
    if plan is None:
        unfold(size, place_ref, arrays, panel)
    copies = []
    for index, (b, array, source, height, base, period, step) in enumerate(plan or ()):
        slot = lax.rem(row + (size - step), size)
        start = pl.multiple_of(base + slot * period, math.gcd(base, period, 16))
        copies.append(
            pltpu.make_async_copy(
                arrays[array].at[pl.ds(source, height), :],
                panel.at[b, pl.ds(start, height), :],
                sem.at[index],
            )
        )
    for copy in copies:
        copy.start()
    for copy in copies:
        copy.wait()

    bit_x = lax.rem(me, 2)
    bit_y = lax.div(me, 2)
    quarter = nb // 4
    base = half + quarter
    upper = jnp.zeros((half, nb), F32)
    lower = jnp.zeros((quarter, nb), F32)
    for b in range(4):
        low, mid = b * nb, b * nb + half
        part = panel[b, 0:half, :]
        upper = upper + part.astype(F32)
        raw[low:mid, low : low + nb] = part
        raw[mid : mid + half, low:mid] = part[:, half:].T
        part = panel[b, half:base, :]
        lower = lower + part.astype(F32)
        raw[mid : mid + quarter, mid : mid + half] = part[:, 0:half]
        raw[mid + quarter : mid + half, mid : mid + half] = part[:, half:]
        own_x = bit_x ^ (b & 1)
        own_y = bit_y ^ (b >> 1)
        pairs = ((own_x, b ^ 1, b), (own_y, b ^ 2, b), (own_y, b ^ 2, b ^ 1))
        for index, (flag, high, low) in enumerate(pairs):
            part = panel[b, base + index * half : base + (index + 1) * half, :]
            tall = jnp.where(flag == 0, high, low)
            wide = jnp.where(flag == 0, low, high)
            rows = pl.multiple_of(tall * nb + flag * half, half)
            cols = pl.multiple_of(wide * nb, nb)
            raw[pl.ds(rows, half), pl.ds(cols, nb)] = part
            raw[pl.ds(cols, nb), pl.ds(rows, half)] = part.T

    def from_diagonal(value):
        r = lax.broadcasted_iota(jnp.int32, value.shape, 0)
        c = lax.broadcasted_iota(jnp.int32, value.shape, 1)
        kept = (c == r) | ((c == r + half + quarter) & (value.shape[0] == quarter))
        return jnp.sum(jnp.where(kept, value, 0.0), keepdims=True)

    trace = from_diagonal(upper) + from_diagonal(lower)

    band = 64
    bands = 9 * quarter // band
    lane = lax.broadcasted_iota(jnp.int32, (1, nb), 1)
    mixed = jnp.where(lane < half, 1.0, 2.0)

    def add_square(index, total):
        start = pl.multiple_of(lax.rem(index, bands) * band, band)
        part = panel[lax.div(index, bands), pl.ds(start, band), :].astype(F32)
        weight = jnp.where(start < half, mixed, jnp.where(start < base, 1.0, 2.0))
        return total + weight * jnp.sum((part * part).reshape(band // 8, 8, nb), axis=0)

    squares = lax.fori_loop(0, 4 * bands, add_square, jnp.zeros((8, nb), F32))
    second = jnp.sum(squares, keepdims=True)
    ratio = SAFETY * (second + 1.0) / (trace + 1.0)
    inverse = 1.0 / ratio
    scale = lax.rsqrt(ratio)

    cells = [(i, j) for j in range(edge) for i in range(j, edge)]

    def place(cell):
        i = jnp.int32(0)
        j = jnp.int32(0)
        for index, (a, b) in enumerate(cells):
            i = jnp.where(cell == index, a, i)
            j = jnp.where(cell == index, b, j)
        rows = pl.ds(pl.multiple_of(i * tile, tile), tile)
        return rows, pl.ds(pl.multiple_of(j * tile, tile), tile)

    def product(left, right, into, linear, quad):
        def multiply(cell, acc):
            rows, cols = place(cell)
            acc[...] = dot(left[rows, :], right[:, cols])

        def finish(cell, acc):
            rows, cols = place(cell)
            value = linear * left[rows, cols].astype(F32) + quad * acc[...]
            value = value.astype(BF16)
            into[rows, cols] = value
            into[cols, rows] = value.T

        def pair(k, carry):
            multiply(2 * k, acc_a)
            finish(2 * k - 1, acc_b)
            multiply(2 * k + 1, acc_b)
            finish(2 * k, acc_a)
            return carry

        def single(cell, carry):
            multiply(cell, acc_a)
            finish(cell, acc_a)
            return carry

        count = len(cells)
        if count % 2:
            lax.fori_loop(0, count, single, 0)
        else:
            lax.fori_loop(0, count // 2, pair, 0)
            finish(count - 1, acc_b)

    acc_b[...] = jnp.zeros_like(acc_b)
    product(raw, raw, one, COEF_THREE * inverse, COEF_FIVE * inverse * inverse)
    product(raw, one, two, COEF_ONE * inverse, inverse)
    product(two, one, raw, COEF_ONE, 1.0)
    product(raw, raw, two, COEF_THREE, COEF_FIVE)
    product(raw, two, three, COEF_ONE, 1.0)

    unit = jnp.where(
        lax.broadcasted_iota(jnp.int32, (nb, nb), 0)
        == lax.broadcasted_iota(jnp.int32, (nb, nb), 1),
        COEF_ONE,
        0.0,
    )

    def column(matrix, source, into, finish):
        def body(i, carry):
            rows = pl.ds(pl.multiple_of(i * tile, tile), tile)
            into[rows, :] = finish(dot(matrix[rows, :], source[...]), rows).astype(BF16)
            return carry

        lax.fori_loop(0, edge, body, 0)

    col_a[...] = two[:, 0:nb]
    col_a[0:nb, :] = (col_a[0:nb, :].astype(F32) + unit).astype(BF16)
    column(three, col_a, col_c, lambda acc, rows: acc)
    column(two, col_c, col_b, lambda acc, rows: COEF_ONE * col_c[rows, :].astype(F32) + acc)
    column(
        three,
        col_b,
        col_a,
        lambda acc, rows: COEF_THREE * col_c[rows, :].astype(F32) + COEF_FIVE * acc,
    )
    col_a[0:nb, :] = (col_a[0:nb, :].astype(F32) + unit).astype(BF16)
    column(two, col_a, col_b, lambda acc, rows: COEF_ONE * col_a[rows, :].astype(F32) + acc)
    column(
        one,
        col_b,
        out_ref,
        lambda acc, rows: scale * (COEF_ONE * col_b[rows, :].astype(F32) + acc),
    )


def chain(plan, arrays, place, size, n):
    nb = n // 4
    tile = min(n, 512)
    flops = int(5.0 * 2 * n**3)
    return pl.pallas_call(
        functools.partial(chain_kernel, plan, size, tile),
        out_shape=jax.ShapeDtypeStruct((n, nb), BF16),
        in_specs=[pl.BlockSpec(memory_space=pltpu.SMEM)]
        + [pl.BlockSpec(memory_space=pl.ANY if plan else pltpu.VMEM)] * len(arrays),
        out_specs=pl.BlockSpec(memory_space=pltpu.VMEM),
        scratch_shapes=[
            pltpu.VMEM((4, 9 * nb // 4, nb), BF16),
            *[pltpu.VMEM((n, n), BF16)] * 4,
            *[pltpu.VMEM((n, nb), BF16)] * 3,
            *[pltpu.VMEM((tile, tile), F32)] * 2,
            pltpu.SemaphoreType.DMA((len(plan or (0,)),)),
        ],
        compiler_params=pltpu.CompilerParams(
            vmem_limit_bytes=min(56, 8 + 24 * n * n // 2**20 // 2) * 2**20
        ),
        cost_estimate=pl.CostEstimate(flops=flops, bytes_accessed=6 * n * nb, transcendentals=0),
    )(place, *arrays)


def apply_kernel(a_ref, b_ref, c_ref, d_ref, q_ref, out_ref):
    nb = a_ref.shape[1]
    total = dot(a_ref[...], q_ref[0:nb, :])
    for index, ref in enumerate((b_ref, c_ref, d_ref)):
        total = total + dot(ref[...], q_ref[(index + 1) * nb : (index + 2) * nb, :])
    out_ref[...] = total.astype(BF16)


def apply(blocks, q):
    rows, nb = blocks[0].shape
    step = rows // 2 if rows % 32 == 0 else rows
    block = pl.BlockSpec((step, nb), lambda i: (i, 0))
    return pl.pallas_call(
        apply_kernel,
        grid=(rows // step,),
        in_specs=[block] * 4 + [pl.BlockSpec((4 * nb, nb), lambda i: (0, 0))],
        out_specs=block,
        out_shape=jax.ShapeDtypeStruct((rows, nb), BF16),
        compiler_params=pltpu.CompilerParams(vmem_limit_bytes=16 * 2**20),
        cost_estimate=pl.CostEstimate(
            flops=8 * rows * nb * nb, bytes_accessed=18 * rows * nb, transcendentals=0
        ),
    )(*blocks, q)


def own_kernel(*refs):
    out_ref = refs[-1]
    total = None
    for ref in refs[:-1]:
        value = ref[...]
        part = dot(value.T, value)
        total = part if total is None else total + part
    total = total.astype(BF16)
    half = total.shape[0] // 2
    base = half + half // 2
    out_ref[0:half, :] = total[0:half]
    out_ref[half:base, 0:half] = total[half:base, half:]
    out_ref[half:base, half:] = total[base:, half:]


def own_gram(blocks):
    nb = blocks[0].shape[1]
    flops = sum(2 * block.shape[0] * nb * nb for block in blocks)
    return pl.pallas_call(
        own_kernel,
        out_shape=jax.ShapeDtypeStruct((3 * nb // 4, nb), BF16),
        compiler_params=pltpu.CompilerParams(vmem_limit_bytes=16 * 2**20),
        cost_estimate=pl.CostEstimate(flops=flops, bytes_accessed=2**20, transcendentals=0),
    )(*blocks)


def cross_kernel(count, place_ref, *refs):
    own, along_x, along_y = refs[0:count], refs[count : 2 * count], refs[2 * count : 3 * count]
    out_ref = refs[-1]
    half = out_ref.shape[1] // 2
    bit_x = lax.rem(place_ref[0], 2)
    bit_y = lax.div(place_ref[0], 2)

    def part(index, left, column, right):
        total = None
        for l_ref, r_ref in zip(left, right):
            value = dot(l_ref[:, column * half : (column + 1) * half].T, r_ref[...])
            total = value if total is None else total + value
        out_ref[index * half : (index + 1) * half, :] = total.astype(BF16)

    @pl.when(bit_x == 0)
    def _():
        part(0, along_x, 0, own)

    @pl.when(bit_x == 1)
    def _():
        part(0, own, 1, along_x)

    @pl.when(bit_y == 0)
    def _():
        part(1, along_y, 0, own)
        part(2, along_y, 0, along_x)

    @pl.when(bit_y == 1)
    def _():
        part(1, own, 1, along_y)
        part(2, along_x, 1, along_y)


def cross_gram(own, along_x, along_y, place):
    nb = own[0].shape[1]
    arrays = (*own, *along_x, *along_y)
    flops = sum(3 * block.shape[0] * nb * nb for block in own)
    return pl.pallas_call(
        functools.partial(cross_kernel, len(own)),
        out_shape=jax.ShapeDtypeStruct((3 * nb // 2, nb), BF16),
        in_specs=[pl.BlockSpec(memory_space=pltpu.SMEM)]
        + [pl.BlockSpec(memory_space=pltpu.VMEM)] * len(arrays),
        out_specs=pl.BlockSpec(memory_space=pltpu.VMEM),
        compiler_params=pltpu.CompilerParams(vmem_limit_bytes=24 * 2**20),
        cost_estimate=pl.CostEstimate(flops=flops, bytes_accessed=2**20, transcendentals=0),
    )(place, *arrays)


def scatter(chunk, size, place):
    return [
        lax.ppermute(chunk(lax.rem(place + step, size)), "fs", shift(size, step))
        for step in range(1, size)
    ]


def add_up(own, moved):
    total = own.astype(F32)
    for value in moved:
        total = total + value.astype(F32)
    return total.astype(BF16)


def spread(piece, size):
    return [lax.ppermute(piece, "fs", shift(size, step)) for step in range(1, size)]


def around(value):
    return [value] + [lax.ppermute(value, "tp", swap(4, b)) for b in (1, 2, 3)]


def pack_kernel(part, *refs):
    values = refs[:-2]
    out_ref = refs[-1]
    count = len(values)
    tail = values[0].shape[0] - part
    for index, ref in enumerate(values):
        out_ref[index * part : (index + 1) * part, :] = ref[0:part, :]
        if tail:
            start = count * part + (count - 1 - index) * tail
            out_ref[start : start + tail, :] = ref[part:, :]


def pack(values, later, part):
    rows = sum(value.shape[0] for value in values)
    return pl.pallas_call(
        functools.partial(pack_kernel, part),
        out_shape=jax.ShapeDtypeStruct((rows, values[0].shape[1]), BF16),
        in_specs=[pl.BlockSpec(memory_space=pltpu.VMEM)] * len(values)
        + [pl.BlockSpec(memory_space=pl.ANY)],
        out_specs=pl.BlockSpec(memory_space=pltpu.VMEM),
        compiler_params=pltpu.CompilerParams(vmem_limit_bytes=16 * 2**20),
    )(*values, later)


def relay(value, split):
    along_x = lax.ppermute(value, "tp", swap(4, 1))
    along_y = lax.ppermute(value, "tp", swap(4, 2))
    upper, lower = along_y[:split], along_x[split:]
    upper = lax.ppermute(upper, "tp", swap(4, 1))
    lower = lax.ppermute(lower, "tp", swap(4, 2))
    return [value, along_x, along_y, upper, lower]


def half_sum(grads, rep):
    height = grads.shape[1] // 2
    theirs = lax.dynamic_slice_in_dim(grads[0], (1 - rep) * height, height, 0)
    mine = lax.dynamic_slice_in_dim(grads[0], rep * height, height, 0)
    return mine, theirs.astype(BF16)


def local(f_size, *arrays):
    return update(f_size, *arrays)


def update(f_size, *arrays):
    rep = lax.axis_index("rep")
    tp = lax.axis_index("tp")
    fs = lax.axis_index("fs")
    place = jnp.stack([tp, fs, rep]).astype(jnp.int32)
    velocities = arrays[1::3]
    weights = arrays[2::3]
    heights = [arrays[3 * k].shape[1] * f_size for k in range(3)]
    cross = swap(2, 1)

    halves = [half_sum(arrays[3 * k], rep) for k in range(3)]
    received = [lax.ppermute(halves[k][1], "rep", cross) for k in range(3)]
    moments = [
        MOMENT * velocities[k] + (halves[k][0] + received[k].astype(F32)) for k in range(3)
    ]
    starts = [moment.astype(BF16) for moment in moments]
    small = starts[2]

    keep = jnp.where(rep == 0, starts[0], starts[1])
    give = jnp.where(rep == 0, starts[1], starts[0])
    small_x = lax.ppermute(small, "tp", swap(4, 1))
    small_y = lax.ppermute(small, "tp", swap(4, 2))
    small_d = lax.ppermute(small, "tp", swap(4, 3))
    keep_x = lax.ppermute(keep, "tp", swap(4, 1))
    keep_y = lax.ppermute(keep, "tp", swap(4, 2))
    gift = lax.ppermute(give, "rep", cross)
    gift_x = lax.ppermute(gift, "tp", swap(4, 1))
    gift_y = lax.ppermute(gift, "tp", swap(4, 2))

    small_panel = jnp.concatenate(
        [own_gram([small]), cross_gram([small], [small_x], [small_y], place)], axis=0
    )
    height = small_panel.shape[0] // 2
    fold = height // 2
    mine = lax.dynamic_slice_in_dim(small_panel, rep * height, height, 0)
    theirs = lax.dynamic_slice_in_dim(small_panel, (1 - rep) * height, height, 0)
    mine = mine.astype(F32) + lax.ppermute(theirs, "rep", cross).astype(F32)
    mine = mine.astype(BF16)
    mine = jnp.concatenate([mine[:fold], mine[fold:]], axis=1)
    diagonal = own_gram([keep, gift])
    nb = diagonal.shape[1]
    base = diagonal.shape[0]
    part = base // f_size
    tail = fold // f_size

    def chunk(index):
        return jnp.concatenate(
            [
                lax.dynamic_slice_in_dim(diagonal, index * part, part, 0),
                lax.dynamic_slice_in_dim(mine, index * tail, tail, 0),
            ],
            axis=0,
        )

    total = add_up(chunk(fs), scatter(chunk, f_size, fs))
    parts = [total] + spread(total, f_size)
    rest = cross_gram([keep, gift], [keep_x, gift_x], [keep_y, gift_y], place)
    height = rest.shape[0] // f_size

    def slab(index):
        return lax.dynamic_slice_in_dim(rest, index * height, height, 0)

    moved = scatter(slab, f_size, fs)
    first_parts = pack(parts, rest, part)
    piece = add_up(slab(fs), moved)
    split = first_parts.shape[0] // 32 * 16
    first_groups = relay(first_parts, split)
    rest_parts = spread(piece, f_size)
    own_groups = around(piece)
    rest_parts = pack(rest_parts, piece, height)
    rest_groups = around(rest_parts)
    spreads = jnp.stack(
        [group[base:] for group in first_groups[:3]] + [first_groups[4][base - split :]]
    )
    others = lax.ppermute(spreads, "rep", cross)
    n = 4 * small.shape[1]
    small_q = chain(None, [spreads, others], place, f_size, n)
    small_out = apply([small, small_x, small_y, small_d], small_q)

    own_groups, rest_groups, first_groups, small_out, keep, gift = lax.optimization_barrier(
        (own_groups, rest_groups, first_groups, small_out, keep, gift)
    )
    n = 4 * nb
    plan = []
    for b in range(4):
        for step in range(f_size):
            low, high = step * part, (step + 1) * part
            if b < 3 or high <= split:
                plan.append((b, b, low, part, 0, part, step))
            elif low >= split:
                plan.append((b, 4, low - split, part, 0, part, step))
            else:
                plan.append((b, 3, low, split - low, 0, part, step))
                plan.append((b, 4, 0, high - split, split - low, part, step))
        plan.append((b, 5 + b, 0, height, base, height, 0))
        for step in range(1, f_size):
            plan.append((b, 9 + b, (step - 1) * height, height, base, height, step))
    both_q = chain(plan, [*first_groups, *own_groups, *rest_groups], place, f_size, n)

    gift_d = lax.ppermute(gift, "tp", swap(4, 3))
    keep_d = lax.ppermute(keep, "tp", swap(4, 3))
    sent = apply([gift, gift_x, gift_y, gift_d], both_q)
    arrived = lax.ppermute(sent, "rep", cross)
    kept = apply([keep, keep_x, keep_y, keep_d], both_q)
    finals = (
        jnp.where(rep == 0, kept, arrived),
        jnp.where(rep == 0, arrived, kept),
        small_out,
    )
    results = []
    for moment, final, weight, rows in zip(moments, finals, weights, heights):
        results.append(moment)
        results.append(SHRINK * weight - RATE * math.sqrt(rows) * final.astype(F32))
    return tuple(results)


def solution(mesh):
    grads = P("rep", "fs", "tp")
    state = P(("fs", "rep"), "tp")
    f_size = mesh.shape["fs"]
    return jax.shard_map(
        functools.partial(local, f_size),
        mesh=mesh,
        in_specs=(grads, state, state) * 3,
        out_specs=(state,) * 6,
        check_vma=False,
    )
```

```python
import functools
import math

import jax
import jax.numpy as jnp
from jax import lax
from jax.experimental import pallas as pl
from jax.experimental.pallas import tpu as pltpu
from jax.sharding import PartitionSpec as P


MOMENT = 0.95
COEF_ONE = 3.4445
COEF_THREE = -4.775
COEF_FIVE = 2.0315
SAFETY = 2.0
RATE = 0.5
SHRINK = 0.95


BF16 = jnp.bfloat16
F32 = jnp.float32


def swap(size, bit):
    return [(i, i ^ bit) for i in range(size)]


def shift(size, step):
    return [(i, (i + step) % size) for i in range(size)]


def dot(left, right):
    return jnp.dot(left, right, preferred_element_type=F32)


def unfold(size, place_ref, arrays, panel):
    rep = place_ref[2]
    fold = arrays[0].shape[1]
    nb = panel.shape[2]
    turn = (place_ref[1] + 1) * (fold // size)
    for array, side in ((arrays[0], rep), (arrays[1], 1 - rep)):
        for b in range(4):
            value = pltpu.roll(array[b].astype(F32), turn, 0).astype(BF16)
            for half in range(2):
                start = pl.multiple_of((2 * side + half) * fold, 16)
                panel[b, pl.ds(start, fold), :] = value[:, half * nb : (half + 1) * nb]


def chain_kernel(plan, size, tile, place_ref, *refs):
    arrays = refs[:-12]
    out_ref, panel, raw, one, two, three, col_a, col_b, col_c, acc_a, acc_b, sem = refs[-12:]
    n = raw.shape[0]
    nb = n // 4
    half = nb // 2
    edge = n // tile
    me = place_ref[0]
    row = place_ref[1]
    if plan is None:
        unfold(size, place_ref, arrays, panel)
    copies = []
    for index, (b, array, source, height, base, period, step) in enumerate(plan or ()):
        slot = lax.rem(row + (size - step), size)
        start = pl.multiple_of(base + slot * period, math.gcd(base, period, 16))
        copies.append(
            pltpu.make_async_copy(
                arrays[array].at[pl.ds(source, height), :],
                panel.at[b, pl.ds(start, height), :],
                sem.at[index],
            )
        )
    for copy in copies:
        copy.start()
    for copy in copies:
        copy.wait()

    bit_x = lax.rem(me, 2)
    bit_y = lax.div(me, 2)
    quarter = nb // 4
    base = half + quarter
    upper = jnp.zeros((half, nb), F32)
    lower = jnp.zeros((quarter, nb), F32)
    for b in range(4):
        low, mid = b * nb, b * nb + half
        part = panel[b, 0:half, :]
        upper = upper + part.astype(F32)
        raw[low:mid, low : low + nb] = part
        raw[mid : mid + half, low:mid] = part[:, half:].T
        part = panel[b, half:base, :]
        lower = lower + part.astype(F32)
        raw[mid : mid + quarter, mid : mid + half] = part[:, 0:half]
        raw[mid + quarter : mid + half, mid : mid + half] = part[:, half:]
        own_x = bit_x ^ (b & 1)
        own_y = bit_y ^ (b >> 1)
        pairs = ((own_x, b ^ 1, b), (own_y, b ^ 2, b), (own_y, b ^ 2, b ^ 1))
        for index, (flag, high, low) in enumerate(pairs):
            part = panel[b, base + index * half : base + (index + 1) * half, :]
            tall = jnp.where(flag == 0, high, low)
            wide = jnp.where(flag == 0, low, high)
            rows = pl.multiple_of(tall * nb + flag * half, half)
            cols = pl.multiple_of(wide * nb, nb)
            raw[pl.ds(rows, half), pl.ds(cols, nb)] = part
            raw[pl.ds(cols, nb), pl.ds(rows, half)] = part.T

    def from_diagonal(value):
        r = lax.broadcasted_iota(jnp.int32, value.shape, 0)
        c = lax.broadcasted_iota(jnp.int32, value.shape, 1)
        kept = (c == r) | ((c == r + half + quarter) & (value.shape[0] == quarter))
        return jnp.sum(jnp.where(kept, value, 0.0), keepdims=True)

    trace = from_diagonal(upper) + from_diagonal(lower)

    band = 64
    bands = 9 * quarter // band
    lane = lax.broadcasted_iota(jnp.int32, (1, nb), 1)
    mixed = jnp.where(lane < half, 1.0, 2.0)

    def add_square(index, total):
        start = pl.multiple_of(lax.rem(index, bands) * band, band)
        part = panel[lax.div(index, bands), pl.ds(start, band), :].astype(F32)
        weight = jnp.where(start < half, mixed, jnp.where(start < base, 1.0, 2.0))
        return total + weight * jnp.sum((part * part).reshape(band // 8, 8, nb), axis=0)

    squares = lax.fori_loop(0, 4 * bands, add_square, jnp.zeros((8, nb), F32))
    second = jnp.sum(squares, keepdims=True)
    ratio = SAFETY * (second + 1.0) / (trace + 1.0)
    inverse = 1.0 / ratio
    scale = lax.rsqrt(ratio)

    cells = [(i, j) for j in range(edge) for i in range(j, edge)]

    def place(cell):
        i = jnp.int32(0)
        j = jnp.int32(0)
        for index, (a, b) in enumerate(cells):
            i = jnp.where(cell == index, a, i)
            j = jnp.where(cell == index, b, j)
        rows = pl.ds(pl.multiple_of(i * tile, tile), tile)
        return rows, pl.ds(pl.multiple_of(j * tile, tile), tile)

    def product(left, right, into, linear, quad):
        def multiply(cell, acc):
            rows, cols = place(cell)
            acc[...] = dot(left[rows, :], right[:, cols])

        def finish(cell, acc):
            rows, cols = place(cell)
            value = linear * left[rows, cols].astype(F32) + quad * acc[...]
            value = value.astype(BF16)
            into[rows, cols] = value
            into[cols, rows] = value.T

        def pair(k, carry):
            multiply(2 * k, acc_a)
            finish(2 * k - 1, acc_b)
            multiply(2 * k + 1, acc_b)
            finish(2 * k, acc_a)
            return carry

        def single(cell, carry):
            multiply(cell, acc_a)
            finish(cell, acc_a)
            return carry

        count = len(cells)
        if count % 2:
            lax.fori_loop(0, count, single, 0)
        else:
            lax.fori_loop(0, count // 2, pair, 0)
            finish(count - 1, acc_b)

    acc_b[...] = jnp.zeros_like(acc_b)
    product(raw, raw, one, COEF_THREE * inverse, COEF_FIVE * inverse * inverse)
    product(raw, one, two, COEF_ONE * inverse, inverse)
    product(two, one, raw, COEF_ONE, 1.0)
    product(raw, raw, two, COEF_THREE, COEF_FIVE)
    product(raw, two, three, COEF_ONE, 1.0)

    unit = jnp.where(
        lax.broadcasted_iota(jnp.int32, (nb, nb), 0)
        == lax.broadcasted_iota(jnp.int32, (nb, nb), 1),
        COEF_ONE,
        0.0,
    )

    def column(matrix, source, into, finish):
        def body(i, carry):
            rows = pl.ds(pl.multiple_of(i * tile, tile), tile)
            into[rows, :] = finish(dot(matrix[rows, :], source[...]), rows).astype(BF16)
            return carry

        lax.fori_loop(0, edge, body, 0)

    col_a[...] = two[:, 0:nb]
    col_a[0:nb, :] = (col_a[0:nb, :].astype(F32) + unit).astype(BF16)
    column(three, col_a, col_c, lambda acc, rows: acc)
    column(two, col_c, col_b, lambda acc, rows: COEF_ONE * col_c[rows, :].astype(F32) + acc)
    column(
        three,
        col_b,
        col_a,
        lambda acc, rows: COEF_THREE * col_c[rows, :].astype(F32) + COEF_FIVE * acc,
    )
    col_a[0:nb, :] = (col_a[0:nb, :].astype(F32) + unit).astype(BF16)
    column(two, col_a, col_b, lambda acc, rows: COEF_ONE * col_a[rows, :].astype(F32) + acc)
    column(
        one,
        col_b,
        out_ref,
        lambda acc, rows: scale * (COEF_ONE * col_b[rows, :].astype(F32) + acc),
    )


def chain(plan, arrays, place, size, n):
    nb = n // 4
    tile = min(n, 512)
    flops = int(5.0 * 2 * n**3)
    return pl.pallas_call(
        functools.partial(chain_kernel, plan, size, tile),
        out_shape=jax.ShapeDtypeStruct((n, nb), BF16),
        in_specs=[pl.BlockSpec(memory_space=pltpu.SMEM)]
        + [pl.BlockSpec(memory_space=pl.ANY if plan else pltpu.VMEM)] * len(arrays),
        out_specs=pl.BlockSpec(memory_space=pltpu.VMEM),
        scratch_shapes=[
            pltpu.VMEM((4, 9 * nb // 4, nb), BF16),
            *[pltpu.VMEM((n, n), BF16)] * 4,
            *[pltpu.VMEM((n, nb), BF16)] * 3,
            *[pltpu.VMEM((tile, tile), F32)] * 2,
            pltpu.SemaphoreType.DMA((len(plan or (0,)),)),
        ],
        compiler_params=pltpu.CompilerParams(
            vmem_limit_bytes=min(56, 8 + 24 * n * n // 2**20 // 2) * 2**20
        ),
        cost_estimate=pl.CostEstimate(flops=flops, bytes_accessed=6 * n * nb, transcendentals=0),
    )(place, *arrays)


def apply_kernel(a_ref, b_ref, c_ref, d_ref, q_ref, out_ref):
    nb = a_ref.shape[1]
    total = dot(a_ref[...], q_ref[0:nb, :])
    for index, ref in enumerate((b_ref, c_ref, d_ref)):
        total = total + dot(ref[...], q_ref[(index + 1) * nb : (index + 2) * nb, :])
    out_ref[...] = total.astype(BF16)


def apply(blocks, q, skip=0):
    rows, nb = blocks[0].shape
    step = rows // 2 if rows % 32 == 0 else rows
    block = pl.BlockSpec((step, nb), lambda i: (i, 0))
    return pl.pallas_call(
        apply_kernel,
        grid=(rows // step,),
        in_specs=[block] * 3
        + [
            pl.BlockSpec((step, nb), lambda i: (i + skip * rows // step, 0)),
            pl.BlockSpec((4 * nb, nb), lambda i: (0, 0)),
        ],
        out_specs=block,
        out_shape=jax.ShapeDtypeStruct((rows, nb), BF16),
        compiler_params=pltpu.CompilerParams(vmem_limit_bytes=16 * 2**20),
        cost_estimate=pl.CostEstimate(
            flops=8 * rows * nb * nb, bytes_accessed=18 * rows * nb, transcendentals=0
        ),
    )(*blocks, q)


def own_kernel(*refs):
    out_ref = refs[-1]
    total = None
    for ref in refs[:-1]:
        value = ref[...]
        part = dot(value.T, value)
        total = part if total is None else total + part
    total = total.astype(BF16)
    half = total.shape[0] // 2
    base = half + half // 2
    out_ref[0:half, :] = total[0:half]
    out_ref[half:base, 0:half] = total[half:base, half:]
    out_ref[half:base, half:] = total[base:, half:]


def own_gram(blocks):
    nb = blocks[0].shape[1]
    flops = sum(2 * block.shape[0] * nb * nb for block in blocks)
    return pl.pallas_call(
        own_kernel,
        out_shape=jax.ShapeDtypeStruct((3 * nb // 4, nb), BF16),
        compiler_params=pltpu.CompilerParams(vmem_limit_bytes=16 * 2**20),
        cost_estimate=pl.CostEstimate(flops=flops, bytes_accessed=2**20, transcendentals=0),
    )(*blocks)


def cross_kernel(count, place_ref, *refs):
    own, along_x, along_y = refs[0:count], refs[count : 2 * count], refs[2 * count : 3 * count]
    out_ref = refs[-1]
    half = out_ref.shape[1] // 2
    bit_x = lax.rem(place_ref[0], 2)
    bit_y = lax.div(place_ref[0], 2)

    def part(index, left, column, right):
        total = None
        for l_ref, r_ref in zip(left, right):
            value = dot(l_ref[:, column * half : (column + 1) * half].T, r_ref[...])
            total = value if total is None else total + value
        out_ref[index * half : (index + 1) * half, :] = total.astype(BF16)

    @pl.when(bit_x == 0)
    def _():
        part(0, along_x, 0, own)

    @pl.when(bit_x == 1)
    def _():
        part(0, own, 1, along_x)

    @pl.when(bit_y == 0)
    def _():
        part(1, along_y, 0, own)
        part(2, along_y, 0, along_x)

    @pl.when(bit_y == 1)
    def _():
        part(1, own, 1, along_y)
        part(2, along_x, 1, along_y)


def cross_gram(own, along_x, along_y, place):
    nb = own[0].shape[1]
    arrays = (*own, *along_x, *along_y)
    flops = sum(3 * block.shape[0] * nb * nb for block in own)
    return pl.pallas_call(
        functools.partial(cross_kernel, len(own)),
        out_shape=jax.ShapeDtypeStruct((3 * nb // 2, nb), BF16),
        in_specs=[pl.BlockSpec(memory_space=pltpu.SMEM)]
        + [pl.BlockSpec(memory_space=pltpu.VMEM)] * len(arrays),
        out_specs=pl.BlockSpec(memory_space=pltpu.VMEM),
        compiler_params=pltpu.CompilerParams(vmem_limit_bytes=24 * 2**20),
        cost_estimate=pl.CostEstimate(flops=flops, bytes_accessed=2**20, transcendentals=0),
    )(place, *arrays)


def scatter(chunk, size, place):
    return [
        lax.ppermute(chunk(lax.rem(place + step, size)), "fs", shift(size, step))
        for step in range(1, size)
    ]


def add_up(own, moved):
    total = own.astype(F32)
    for value in moved:
        total = total + value.astype(F32)
    return total.astype(BF16)


def spread(piece, size):
    return [lax.ppermute(piece, "fs", shift(size, step)) for step in range(1, size)]


def around(value):
    return [value] + [lax.ppermute(value, "tp", swap(4, b)) for b in (1, 2, 3)]


def pack_kernel(part, *refs):
    values = refs[:-2]
    out_ref = refs[-1]
    count = len(values)
    tail = values[0].shape[0] - part
    for index, ref in enumerate(values):
        out_ref[index * part : (index + 1) * part, :] = ref[0:part, :]
        if tail:
            start = count * part + (count - 1 - index) * tail
            out_ref[start : start + tail, :] = ref[part:, :]


def pack(values, later, part):
    rows = sum(value.shape[0] for value in values)
    return pl.pallas_call(
        functools.partial(pack_kernel, part),
        out_shape=jax.ShapeDtypeStruct((rows, values[0].shape[1]), BF16),
        in_specs=[pl.BlockSpec(memory_space=pltpu.VMEM)] * len(values)
        + [pl.BlockSpec(memory_space=pl.ANY)],
        out_specs=pl.BlockSpec(memory_space=pltpu.VMEM),
        compiler_params=pltpu.CompilerParams(vmem_limit_bytes=16 * 2**20),
    )(*values, later)


def relay(value, split):
    along_x = lax.ppermute(value, "tp", swap(4, 1))
    along_y = lax.ppermute(value, "tp", swap(4, 2))
    upper, lower = along_y[:split], along_x[split:]
    upper = lax.ppermute(upper, "tp", swap(4, 1))
    lower = lax.ppermute(lower, "tp", swap(4, 2))
    return [value, along_x, along_y, upper, lower]


def half_sum(grads, rep):
    height = grads.shape[1] // 2
    theirs = lax.dynamic_slice_in_dim(grads[0], (1 - rep) * height, height, 0)
    mine = lax.dynamic_slice_in_dim(grads[0], rep * height, height, 0)
    return mine, theirs.astype(BF16)


def local(f_size, *arrays):
    return update(f_size, *arrays)


def update(f_size, *arrays):
    rep = lax.axis_index("rep")
    tp = lax.axis_index("tp")
    fs = lax.axis_index("fs")
    place = jnp.stack([tp, fs, rep]).astype(jnp.int32)
    velocities = arrays[1::3]
    weights = arrays[2::3]
    heights = [arrays[3 * k].shape[1] * f_size for k in range(3)]
    cross = swap(2, 1)

    halves = [half_sum(arrays[3 * k], rep) for k in range(3)]
    received = [lax.ppermute(halves[k][1], "rep", cross) for k in range(3)]
    moments = [
        MOMENT * velocities[k] + (halves[k][0] + received[k].astype(F32)) for k in range(3)
    ]
    starts = [moment.astype(BF16) for moment in moments]
    small = starts[2]

    keep = jnp.where(rep == 0, starts[0], starts[1])
    give = jnp.where(rep == 0, starts[1], starts[0])
    small_x = lax.ppermute(small, "tp", swap(4, 1))
    small_y = lax.ppermute(small, "tp", swap(4, 2))
    small_d = lax.ppermute(small, "tp", swap(4, 3))
    keep_x = lax.ppermute(keep, "tp", swap(4, 1))
    keep_y = lax.ppermute(keep, "tp", swap(4, 2))
    gift = lax.ppermute(give, "rep", cross)
    gift_x = lax.ppermute(gift, "tp", swap(4, 1))
    gift_y = lax.ppermute(gift, "tp", swap(4, 2))

    small_panel = jnp.concatenate(
        [own_gram([small]), cross_gram([small], [small_x], [small_y], place)], axis=0
    )
    height = small_panel.shape[0] // 2
    fold = height // 2
    mine = lax.dynamic_slice_in_dim(small_panel, rep * height, height, 0)
    theirs = lax.dynamic_slice_in_dim(small_panel, (1 - rep) * height, height, 0)
    mine = mine.astype(F32) + lax.ppermute(theirs, "rep", cross).astype(F32)
    mine = mine.astype(BF16)
    mine = jnp.concatenate([mine[:fold], mine[fold:]], axis=1)
    diagonal = own_gram([keep, gift])
    nb = diagonal.shape[1]
    base = diagonal.shape[0]
    part = base // f_size
    tail = fold // f_size

    def chunk(index):
        return jnp.concatenate(
            [
                lax.dynamic_slice_in_dim(diagonal, index * part, part, 0),
                lax.dynamic_slice_in_dim(mine, index * tail, tail, 0),
            ],
            axis=0,
        )

    total = add_up(chunk(fs), scatter(chunk, f_size, fs))
    parts = [total] + spread(total, f_size)
    rest = cross_gram([keep, gift], [keep_x, gift_x], [keep_y, gift_y], place)
    height = rest.shape[0] // f_size

    def slab(index):
        return lax.dynamic_slice_in_dim(rest, index * height, height, 0)

    moved = scatter(slab, f_size, fs)
    first_parts = pack(parts, rest, part)
    piece = add_up(slab(fs), moved)
    split = first_parts.shape[0] // 32 * 16
    first_groups = relay(first_parts, split)
    rest_parts = spread(piece, f_size)
    own_groups = around(piece)
    rest_parts = pack(rest_parts, piece, height)
    rest_groups = around(rest_parts)
    spreads = jnp.stack(
        [group[base:] for group in first_groups[:3]] + [first_groups[4][base - split :]]
    )
    others = lax.ppermute(spreads, "rep", cross)
    n = 4 * small.shape[1]
    small_q = chain(None, [spreads, others], place, f_size, n)
    small_out = apply([small, small_x, small_y, small_d], small_q)

    both = jnp.concatenate([keep, gift], axis=0)
    own_groups, rest_groups, first_groups, small_out, both = lax.optimization_barrier(
        (own_groups, rest_groups, first_groups, small_out, both)
    )
    n = 4 * nb
    plan = []
    for b in range(4):
        for step in range(f_size):
            low, high = step * part, (step + 1) * part
            if b < 3 or high <= split:
                plan.append((b, b, low, part, 0, part, step))
            elif low >= split:
                plan.append((b, 4, low - split, part, 0, part, step))
            else:
                plan.append((b, 3, low, split - low, 0, part, step))
                plan.append((b, 4, 0, high - split, split - low, part, step))
        plan.append((b, 5 + b, 0, height, base, height, 0))
        for step in range(1, f_size):
            plan.append((b, 9 + b, (step - 1) * height, height, base, height, step))
    both_q = chain(plan, [*first_groups, *own_groups, *rest_groups], place, f_size, n)

    both_d = lax.ppermute(both, "tp", swap(4, 3))
    sent = apply([gift, gift_x, gift_y, both_d], both_q, 1)
    arrived = lax.ppermute(sent, "rep", cross)
    kept = apply([keep, keep_x, keep_y, both_d], both_q)
    finals = (
        jnp.where(rep == 0, kept, arrived),
        jnp.where(rep == 0, arrived, kept),
        small_out,
    )
    results = []
    for moment, final, weight, rows in zip(moments, finals, weights, heights):
        results.append(moment)
        results.append(SHRINK * weight - RATE * math.sqrt(rows) * final.astype(F32))
    return tuple(results)


def solution(mesh):
    grads = P("rep", "fs", "tp")
    state = P(("fs", "rep"), "tp")
    f_size = mesh.shape["fs"]
    return jax.shard_map(
        functools.partial(local, f_size),
        mesh=mesh,
        in_specs=(grads, state, state) * 3,
        out_specs=(state,) * 6,
        check_vma=False,
    )
```
